32 devices in a mesh: grp: 2 (over y), sp: 4 (over z), tp: 4 (over x, core).
Axes of the slice: x: 2, y: 2, z: 4, core: 2. Of those that a mesh axis runs over, the one named last changes fastest.
Arguments:
- resid_in: bfloat16 [2048, 2048], P(('grp', 'sp', 'tp')), parts along dimension 0, may hold values from -3 to 3
- queries: bfloat16 [2048, 1024], P(('grp', 'sp'), 'tp'), parts along dimension 0, may hold values from -39 to 39
- keys: bfloat16 [2048, 1024], P(('grp', 'sp'), 'tp'), parts along dimension 0, may hold values from -6 to 6
- values: bfloat16 [2048, 1024], P(('grp', 'sp'), 'tp'), parts along dimension 0, may hold values from -12 to 12
- cum_gate: float32 [2048, 16], P('grp', 'tp'), parts along dimension 0, may hold values from -105 to 0, as said below
- w_out: bfloat16 [1024, 2048], replicated, may hold values from -0.1875 to 0.1875
- norm_gain: float32 [2048], replicated, may hold values from 0.1 to 1.9
- w_gate: bfloat16 [2048, 5632], P('sp', 'tp'), may hold values from -0.125 to 0.125
- w_up: bfloat16 [2048, 5632], P('sp', 'tp'), may hold values from -0.125 to 0.125
- w_down: bfloat16 [5632, 2048], P('tp', 'sp'), may hold values from -0.078125 to 0.078125
Outputs:
- resid_out: bfloat16 [2048, 2048], P(('grp', 'sp', 'tp')), parts along dimension 0
The draws below stay inside these ranges and needn't reach their ends.
There are 2 independent parts, one for each index of `grp`. The reference program is written for one: setup_inputs(seed, part) draws one part's arguments, and reference() takes and returns one part's arrays. A program takes and returns all parts, laid end to end along the dimension named above; an argument that names none is the same for every part. Nothing has to cross between parts.
Inputs may be any that keep to these rules, and one draw needn't show every extreme that they name: `cum_gate`: in every head the values never rise from one position to the next, and the first is at most 0.
All inputs are finite; a program needn't handle non-finite values.
Results may differ from the reference program's by a relative error of at most 0.018.
Values may be sent and summed in bfloat16 or wider, within the bound.
No kernel may reach another device: no remote copies, remote signals or barrier semaphores. Data moves between devices by JAX's collectives and lax.ppermute only.
A program may use at most 128 MiB of HBM per device.

```python
import math
import jax
import jax.numpy as jnp
from jax import lax

D = 2048
HEADS = 16
HEAD_DIM = 64
FF = 5632
TOK_DEV = 256
SEQUENCE_TOKENS = 1024
ATT_WIDTH = 1024


def attention_pair(key):
    key_q, key_k = jax.random.split(key, 2)
    width = HEADS * HEAD_DIM
    queries = 2.0 * jnp.clip(jax.random.normal(key_q, (SEQUENCE_TOKENS, width), jnp.float32), -6.0, 6.0)
    keys = jnp.clip(jax.random.normal(key_k, (SEQUENCE_TOKENS, width), jnp.float32), -6.0, 6.0)
    return (queries, keys)


def draw_queries(key, part):
    return attention_pair(jax.random.fold_in(key, 11))[0].astype(jnp.bfloat16)


def draw_keys(key, part):
    return attention_pair(jax.random.fold_in(key, 11))[1].astype(jnp.bfloat16)


def draw_cum_gate(key, part):
    every_key_row = jax.random.split(jax.random.fold_in(key, 23), 6)
    sluggish_path = jax.random.permutation(every_key_row[0], HEADS) < HEADS // 2
    fast_rate = jnp.exp(jax.random.uniform(every_key_row[1], (HEADS,), jnp.float32, jnp.log(1.0 / 100.0), jnp.log(1.0 / 30.0)))
    rate = jnp.where(sluggish_path, 0.4 / SEQUENCE_TOKENS, fast_rate)
    factor = jnp.exp(jax.random.uniform(every_key_row[2], (SEQUENCE_TOKENS // TOK_DEV, 1), jnp.float32, jnp.log(0.5), jnp.log(2.0)))
    factor = jnp.repeat(factor, TOK_DEV, axis=0)
    rough = jax.random.uniform(every_key_row[3], (SEQUENCE_TOKENS, HEADS), jnp.float32, 0.5, 1.5)
    step_count = -rate[None, :] * factor * rough
    spike_position = jax.random.randint(every_key_row[4], (3,), 1, SEQUENCE_TOKENS, dtype=jnp.int32)
    training_loss = jax.random.uniform(every_key_row[5], (3, HEADS), jnp.float32, 0.2, 0.5)
    step_count = step_count.at[spike_position].add(jnp.log(1.0 - training_loss) * sluggish_path.astype(jnp.float32)[None, :])
    return jnp.cumsum(step_count, axis=0)


def levels(key, shape, cuts, low, top_value):
    factor_of, own = 1.0, jax.random.fold_in(key, 6)
    for position, shards_of in cuts:
        draws = jnp.exp(jax.random.uniform(jax.random.fold_in(own, position), (shards_of,), jnp.float32, low / len(cuts), top_value / len(cuts)))
        factor_of = factor_of * jnp.repeat(draws, shape[position] // shards_of).reshape([-1 if axis == position else 1 for axis in range(len(shape))])
    return factor_of


def scatter_about(key, shape, spread, reach, pieces=(), held_as=jnp.bfloat16):
    gain = levels(key, shape, pieces, -0.22, 0.18) if pieces else 1.0
    drawn = jax.random.normal(key, shape, jnp.float32) * spread * gain
    return jnp.minimum(jnp.maximum(drawn, -reach), reach).astype(held_as)


def setup_inputs(seed: int = 0, part: int = 0) -> dict:
    splits = jax.random.split(jax.random.key(seed), 11)
    part_splits = jax.random.split(jax.random.fold_in(splits[10], part), 11)
    return {
        "resid_in": scatter_about(part_splits[0], (SEQUENCE_TOKENS, D), 0.5, 3.0, ((0, 16),)),
        "queries": draw_queries(jax.random.fold_in(jax.random.fold_in(splits[10], part), 71), part),
        "keys": draw_keys(jax.random.fold_in(jax.random.fold_in(splits[10], part), 71), part),
        "values": scatter_about(part_splits[3], (SEQUENCE_TOKENS, ATT_WIDTH), 2.0, 12.0, ((0, 4), (1, 4))),
        "cum_gate": draw_cum_gate(jax.random.fold_in(jax.random.fold_in(splits[10], part), 71), part),
        "w_out": scatter_about(splits[5], (ATT_WIDTH, D), ATT_WIDTH ** -0.5, 0.1875),
        "norm_gain": jnp.clip(1.0 + 0.18 * jax.random.normal(splits[6], (D,), jnp.float32), 0.1, 1.9),
        "w_gate": scatter_about(splits[7], (D, FF), D ** -0.5, 0.125, ((0, 4), (1, 4))),
        "w_up": scatter_about(splits[8], (D, FF), D ** -0.5, 0.125, ((0, 4), (1, 4))),
        "w_down": scatter_about(splits[9], (FF, D), FF ** -0.5, 0.078125, ((0, 4), (1, 4))),
    }


def attention(queries, keys, values, cum_gate):
    total = queries.shape[0]
    span = math.gcd(total, 256)
    scale = HEAD_DIM ** (-0.5)
    query_heads = queries.astype(jnp.float32).reshape(total, HEADS, HEAD_DIM)
    key_heads = keys.astype(jnp.float32).reshape(total, HEADS, HEAD_DIM)
    value_heads = values.astype(jnp.float32).reshape(total, HEADS, HEAD_DIM)
    positions = jnp.arange(total, dtype=jnp.int32)

    def block(first):
        query_block = lax.dynamic_slice_in_dim(query_heads, first, span, 0)
        gate_block_rows = lax.dynamic_slice_in_dim(cum_gate, first, span, 0)
        scores = jnp.einsum('qhd,khd->hqk', query_block, key_heads) * scale
        scores = scores + gate_block_rows.T[:, :, None] - cum_gate.T[:, None, :]
        mask = positions[None, :] <= (first + jnp.arange(span, dtype=jnp.int32))[:, None]
        scores = jnp.where(mask[None], scores, -1e+30)
        top = lax.optimization_barrier(jnp.max(scores, axis=-1, keepdims=True))
        weights = jnp.where(mask[None], jnp.exp(scores - top), 0.0)
        totals = lax.optimization_barrier(jnp.sum(weights, axis=-1))
        rounded = lax.optimization_barrier(weights.astype(jnp.bfloat16)).astype(jnp.float32)
        attended = jnp.einsum('hqk,khd->qhd', rounded, value_heads) / totals.T[:, :, None]
        return attended.reshape(span, HEADS * HEAD_DIM).astype(jnp.bfloat16)
    starts = jnp.arange(total // span, dtype=jnp.int32) * span
    return lax.map(block, starts).reshape(total, HEADS * HEAD_DIM)

def reference(resid_in, queries, keys, values, cum_gate, w_out, norm_gain, w_gate, w_up, w_down):
    attended = attention(queries, keys, values, cum_gate)
    mixed = jnp.dot(attended, w_out, preferred_element_type=jnp.float32)
    resid = resid_in.astype(jnp.float32) + mixed
    normed = resid * lax.rsqrt(lax.optimization_barrier(jnp.mean(resid * resid, axis=-1, keepdims=True)) + 1e-06)
    normed = (normed * norm_gain).astype(jnp.bfloat16)
    gate = jnp.dot(normed, w_gate, preferred_element_type=jnp.float32)
    up = jnp.dot(normed, w_up, preferred_element_type=jnp.float32)
    hidden = (jax.nn.silu(gate) * up).astype(jnp.bfloat16)
    down = jnp.dot(hidden, w_down, preferred_element_type=jnp.float32)
    return (resid + down).astype(jnp.bfloat16)
```

```python
import math

import jax
import jax.numpy as jnp
from jax import lax
from jax.experimental import pallas as pl
from jax.experimental.pallas import tpu as pltpu
from jax.sharding import PartitionSpec as P

HEAD_DIM = 64
LANES = 128


def gathered(resid_in, queries, keys, values, cum_gate, w_out, norm_gain, w_gate, w_up, w_down):
    tok_rows = queries.shape[0]
    local_heads = queries.shape[1] // HEAD_DIM
    scale = HEAD_DIM ** (-0.5)
    offset = lax.axis_index("sp") * tok_rows
    query_heads = queries.reshape(tok_rows, local_heads, HEAD_DIM)
    own_gate = lax.dynamic_slice_in_dim(cum_gate, offset, tok_rows, 0).T
    query_pos = offset + jnp.arange(tok_rows, dtype=jnp.int32)
    last_pos = offset + tok_rows - 1
    initial = (
        jnp.full((local_heads, tok_rows), -1e30, jnp.float32),
        jnp.zeros((local_heads, tok_rows), jnp.float32),
        jnp.zeros((tok_rows, local_heads, HEAD_DIM), jnp.float32),
    )
    key_piece = lax.all_gather(keys, "sp", axis=0, tiled=True)
    value_piece = lax.all_gather(values, "sp", axis=0, tiled=True)
    length = key_piece.shape[0]
    span = math.gcd(length, 512)

    def block(index, state):
        begin = index * span

        def work(inner):
            maxima, totals, summed = inner
            key_block = lax.dynamic_slice_in_dim(key_piece, index * span, span, 0).reshape(
                span, local_heads, HEAD_DIM
            )
            value_block_rows = lax.dynamic_slice_in_dim(value_piece, index * span, span, 0).reshape(
                span, local_heads, HEAD_DIM
            )
            key_gate = lax.dynamic_slice_in_dim(cum_gate, begin, span, 0).T
            scores = (
                jnp.einsum(
                    "qhd,khd->hqk", query_heads, key_block, preferred_element_type=jnp.float32
                )
                * scale
            )
            scores = scores + own_gate[:, :, None] - key_gate[:, None, :]
            key_pos = begin + jnp.arange(span, dtype=jnp.int32)
            mask = (key_pos[None, :] <= query_pos[:, None])[None]
            scores = jnp.where(mask, scores, -1e30)
            new_max = jnp.maximum(maxima, jnp.max(scores, axis=-1))
            weights = jnp.where(mask, jnp.exp(scores - new_max[:, :, None]), 0.0)
            rescale = jnp.exp(maxima - new_max)
            totals = totals * rescale + jnp.sum(weights, axis=-1)
            product = jnp.einsum(
                "hqk,khd->qhd",
                weights.astype(jnp.bfloat16),
                value_block_rows,
                preferred_element_type=jnp.float32,
            )
            summed = summed * rescale.T[:, :, None] + product
            return (new_max, totals, summed)

        return lax.cond(begin <= last_pos, work, lambda inner: inner, state)

    maxima, totals, summed = lax.fori_loop(0, length // span, block, initial)
    attended = (
        (summed / totals.T[:, :, None])
        .reshape(tok_rows, local_heads * HEAD_DIM)
        .astype(jnp.bfloat16)
    )
    head_rows = lax.all_to_all(attended, "tp", split_axis=0, concat_axis=1, tiled=True)
    mixed = jnp.dot(head_rows, w_out, preferred_element_type=jnp.float32)
    resid = resid_in.astype(jnp.float32) + mixed
    normed = resid * lax.rsqrt(jnp.mean(resid * resid, axis=-1, keepdims=True) + 1e-06)
    normed = (normed * norm_gain).astype(jnp.bfloat16)
    all_rows = lax.all_gather(normed, "tp", axis=0, tiled=True)
    full_gate, full_up, full_down = (
        lax.all_gather(w_gate, "sp", axis=0, tiled=True),
        lax.all_gather(w_up, "sp", axis=0, tiled=True),
        lax.all_gather(w_down, "sp", axis=1, tiled=True),
    )
    gate = jnp.dot(all_rows, full_gate, preferred_element_type=jnp.float32)
    up = jnp.dot(all_rows, full_up, preferred_element_type=jnp.float32)
    hidden = (jax.nn.silu(gate) * up).astype(jnp.bfloat16)
    terms = jnp.dot(hidden, full_down, preferred_element_type=jnp.float32)
    back = lax.psum_scatter(
        terms.astype(jnp.bfloat16), "tp", scatter_dimension=0, tiled=True
    ).astype(jnp.float32)
    return (resid + back).astype(jnp.bfloat16)


def splits(sizes, width, units, depth):
    if sizes["grp"] != 2 or sizes["tp"] != 4 or units % LANES:
        return False
    tiles = units // LANES
    per = -(-tiles // sizes["sp"])
    half = depth // 2
    span = per * LANES
    extra = span - half
    return (
        per * (sizes["sp"] - 1) < tiles
        and depth % (4 * LANES) == 0
        and extra > 0
        and half % extra == 0
        and width == depth * sizes["sp"]
    )


VMEM = pl.BlockSpec(memory_space=pltpu.VMEM)
SMEM = pl.BlockSpec(memory_space=pltpu.SMEM)
ANY = pl.BlockSpec(memory_space=pl.ANY)


def pack(place, w_gate, w_up, w_down, sp, span):
    depth, units = w_gate.shape
    half = depth // 2
    tiles = units // LANES
    per = span // LANES
    extra = span - half

    def body(place_ref, gate_ref, up_ref, down_ref, *rest):
        outs, sem = rest[:sp], rest[sp]
        s, g = place_ref[0], place_ref[1]
        copies = []

        def put(src, dst):
            copy = pltpu.make_async_copy(src, dst, sem)
            copy.start()
            copies.append(copy)

        def piece(out, dest, which):
            start = pl.multiple_of(jnp.minimum(per * dest, tiles - per) * LANES, LANES)
            row = pl.multiple_of(which * half, LANES)
            put(gate_ref.at[pl.ds(row, half), pl.ds(start, span)], out.at[pl.ds(0, half), :])
            put(up_ref.at[pl.ds(row, half), pl.ds(start, span)], out.at[pl.ds(half, half), :])
            put(
                down_ref.at[pl.ds(start, half), pl.ds(row, half)],
                out.at[pl.ds(2 * half, half), pl.ds(0, half)],
            )
            low = pl.multiple_of(start + half, LANES)
            for j in range(half // extra):
                col = pl.multiple_of(row + j * extra, LANES)
                put(
                    down_ref.at[pl.ds(low, extra), pl.ds(col, extra)],
                    out.at[pl.ds(2 * half + j * extra, extra), pl.ds(half, extra)],
                )

        for k in range(1, sp):
            piece(outs[k], lax.rem(s + k, sp), g)
        for which in range(2):
            piece(outs[0].at[which], s, which)
        for copy in copies:
            copy.wait()

    shape = jax.ShapeDtypeStruct((3 * half, span), w_gate.dtype)
    return pl.pallas_call(
        body,
        in_specs=[SMEM, ANY, ANY, ANY],
        out_specs=[ANY] * sp,
        out_shape=[jax.ShapeDtypeStruct((2, 3 * half, span), w_gate.dtype)] + [shape] * (sp - 1),
        scratch_shapes=[pltpu.SemaphoreType.DMA],
        name="pack",
    )(place, w_gate, w_up, w_down)


def attend(place, queries, pairs, cum_gate, gate_rows):
    rows, width = queries.shape
    heads = width // HEAD_DIM
    blocks = len(pairs)
    scale = HEAD_DIM ** (-0.5)

    def body(place_ref, q_ref, *rest):
        pair_refs, cum_ref, gate_ref, out_ref = rest[:blocks], *rest[blocks:]
        s = place_ref[0]
        query = q_ref[...] * jnp.asarray(scale, q_ref.dtype)
        lane = lax.broadcasted_iota(jnp.int32, (rows, width), 1) // HEAD_DIM
        row_id = lax.broadcasted_iota(jnp.int32, (rows, rows), 0)
        col_id = lax.broadcasted_iota(jnp.int32, (rows, rows), 1)
        own = cum_ref[pl.ds(pl.multiple_of(s * rows, LANES), rows), :]
        result = jnp.zeros((rows, width), jnp.float32)
        for h in range(heads):
            one = jnp.where(lane == h, query, jnp.zeros_like(query))
            scores = []
            for k in range(blocks):
                keys = pair_refs[k][0:rows, :]
                score = lax.dot_general(
                    one, keys, (((1,), (1,)), ((), ())), preferred_element_type=jnp.float32
                )
                at = pl.multiple_of(lax.rem(s - k + blocks, blocks) * rows, LANES)
                score = score + own[:, h : h + 1] - gate_ref[h : h + 1, pl.ds(at, rows)]
                keep = (col_id <= row_id) if k == 0 else (jnp.full((1, 1), s - k, jnp.int32) >= 0)
                scores.append(jnp.where(keep, score, -1e30))
            top = scores[0].max(axis=-1, keepdims=True)
            for k in range(1, blocks):
                top = jnp.maximum(top, scores[k].max(axis=-1, keepdims=True))
            total = jnp.zeros((rows, 1), jnp.float32)
            summed = jnp.zeros((rows, width), jnp.float32)
            for k in range(blocks):
                weight = jnp.exp(scores[k] - top)
                total = total + weight.sum(axis=-1, keepdims=True)
                summed = summed + jnp.dot(
                    weight.astype(jnp.bfloat16),
                    pair_refs[k][rows : 2 * rows, :],
                    preferred_element_type=jnp.float32,
                )
            result = jnp.where(lane == h, summed / total, result)
        out_ref[...] = result.astype(out_ref.dtype)

    return pl.pallas_call(
        body,
        in_specs=[SMEM] + [VMEM] * (blocks + 3),
        out_specs=VMEM,
        out_shape=jax.ShapeDtypeStruct((rows, width), jnp.bfloat16),
        name="attend",
    )(place, queries, *pairs, cum_gate, gate_rows)


def feed(place, mine, other, pieces, tiles, span):
    sp = len(mine)
    block, width = mine[0].shape
    depth = width // sp
    half = depth // 2
    extra = span - half
    rows = 2 * sp * block
    cols = 2 * span
    per = span // LANES
    arrays = [p[3] for p in pieces]

    def body(place_ref, *rest):
        row_refs = rest[: 2 * sp]
        piece_refs = rest[2 * sp : 2 * sp + len(arrays)]
        own_ref, other_ref, x_ref, gate_ref, up_ref, down_ref, sems = rest[2 * sp + len(arrays) :]
        s, g = place_ref[0], place_ref[1]
        copies = [[], [], [], []]

        def put(src, dst, n):
            copy = pltpu.make_async_copy(src, dst, sems.at[n])
            copy.start()
            copies[n].append(copy)

        for j, ref in enumerate(row_refs):
            put(ref, x_ref.at[pl.ds(j * block, block), :], 0)

        def spread(stage):
            for (k, which, column, _), ref in zip(pieces, piece_refs, strict=True):
                for n in range(2) if which is None else (which,):
                    src = ref.at[n] if which is None else ref
                    part = n if which is None else (g if n == 0 else 1 - g)
                    at = pl.multiple_of(lax.rem(s - k + sp, sp) * depth + part * half, LANES)
                    col = column * span
                    if stage == 1:
                        put(src.at[pl.ds(0, half), :], gate_ref.at[pl.ds(at, half), pl.ds(col, span)], 1)
                    elif stage == 2:
                        put(src.at[pl.ds(half, half), :], up_ref.at[pl.ds(at, half), pl.ds(col, span)], 2)
                    else:
                        put(
                            src.at[pl.ds(2 * half, half), pl.ds(0, half)],
                            down_ref.at[pl.ds(col, half), pl.ds(at, half)],
                            3,
                        )
                        for j in range(half // extra):
                            put(
                                src.at[pl.ds(2 * half + j * extra, extra), pl.ds(half, extra)],
                                down_ref.at[
                                    pl.ds(col + half, extra),
                                    pl.ds(pl.multiple_of(at + j * extra, LANES), extra),
                                ],
                                3,
                            )

        for stage in (1, 2, 3):
            spread(stage)
        for n in (0, 1):
            for copy in copies[n]:
                copy.wait()
        gate = jnp.dot(x_ref[...], gate_ref[...], preferred_element_type=jnp.float32)
        for copy in copies[2]:
            copy.wait()
        up = jnp.dot(x_ref[...], up_ref[...], preferred_element_type=jnp.float32)
        hidden = gate / (1.0 + jnp.exp(-gate)) * up
        again = per * s - jnp.minimum(per * s, tiles - per)
        unit = lax.broadcasted_iota(jnp.int32, (rows, cols), 1)
        unit = jnp.where(unit >= span, unit - span, unit)
        hidden = jnp.where(unit >= again * LANES, hidden, 0.0).astype(jnp.bfloat16)
        for copy in copies[3]:
            copy.wait()
        product = jnp.dot(hidden, down_ref[...], preferred_element_type=jnp.float32)
        own_ref[...] = product[: rows // 2]
        other_ref[...] = product[rows // 2 :].astype(other_ref.dtype)

    return pl.pallas_call(
        body,
        in_specs=[SMEM] + [ANY] * (2 * sp + len(arrays)),
        out_specs=[VMEM, VMEM],
        out_shape=[
            jax.ShapeDtypeStruct((rows // 2, width), jnp.float32),
            jax.ShapeDtypeStruct((rows // 2, width), jnp.bfloat16),
        ],
        scratch_shapes=[
            pltpu.VMEM((rows, width), jnp.bfloat16),
            pltpu.VMEM((width, cols), jnp.bfloat16),
            pltpu.VMEM((width, cols), jnp.bfloat16),
            pltpu.VMEM((cols, width), jnp.bfloat16),
            pltpu.SemaphoreType.DMA((4,)),
        ],
        name="feed",
    )(place, *mine, *other, *arrays)


def unit_slices(resid_in, queries, keys, values, cum_gate, w_out, norm_gain, w_gate, w_up, w_down):
    sp, tp = lax.axis_size("sp"), lax.axis_size("tp")
    tiles = w_gate.shape[1] // LANES
    span = -(-tiles // sp) * LANES
    place = jnp.stack([lax.axis_index("sp"), lax.axis_index("grp")]).astype(jnp.int32)

    def turn(a, k):
        return lax.ppermute(a, "sp", [(i, (i + k) % sp) for i in range(sp)])

    def later(a, k):
        return lax.ppermute(a, "sp", [(i, i + k) for i in range(sp - k)])

    def flip(a, m):
        return lax.ppermute(a, "tp", [(i, i ^ m) for i in range(tp)])

    def swap(a):
        return lax.ppermute(a, "grp", [(0, 1), (1, 0)])

    across, core = tp // 2, 1
    pair = jnp.concatenate([keys, values], axis=0)
    packed = pack(place, w_gate, w_up, w_down, sp, span)
    pieces = [(0, None, 0, packed[0]), (0, None, 1, flip(packed[0], across))]
    pairs = [pair] + [later(pair, k) for k in range(1, sp)]
    for k in range(1, sp):
        here = turn(packed[k], k)
        there = flip(here, across)
        pieces += [(k, 0, 0, here), (k, 1, 0, swap(here)), (k, 0, 1, there), (k, 1, 1, swap(there))]

    attended = attend(place, queries, pairs, cum_gate, cum_gate.T)
    head_rows = lax.all_to_all(attended, "tp", split_axis=0, concat_axis=1, tiled=True)
    mixed = jnp.dot(head_rows, w_out, preferred_element_type=jnp.float32)
    resid = resid_in.astype(jnp.float32) + mixed
    normed = resid * lax.rsqrt(jnp.mean(resid * resid, axis=-1, keepdims=True) + 1e-06)
    normed = (normed * norm_gain).astype(jnp.bfloat16)

    mine = [normed] + [turn(normed, k) for k in range(1, sp)]
    other = [flip(a, core) for a in mine]
    own, away = feed(place, mine, other, pieces, tiles, span)
    total = own + flip(away, core).astype(jnp.float32)
    total = total.reshape(sp, -1, total.shape[1])
    result = resid + total[0]
    for k in range(1, sp):
        result = result + turn(total[k].astype(jnp.bfloat16), sp - k).astype(jnp.float32)
    return result.astype(jnp.bfloat16)


def on_device(*arrays):
    sizes = {name: lax.axis_size(name) for name in ("grp", "sp", "tp")}
    w_out, w_gate = arrays[5], arrays[7]
    if splits(sizes, w_out.shape[1], w_gate.shape[1], w_gate.shape[0]):
        return unit_slices(*arrays)
    return gathered(*arrays)


def solution(mesh):
    return jax.shard_map(
        on_device,
        mesh=mesh,
        in_specs=(
            P(("grp", "sp", "tp"), None),
            P(("grp", "sp"), "tp"),
            P(("grp", "sp"), "tp"),
            P(("grp", "sp"), "tp"),
            P("grp", "tp"),
            P(),
            P(),
            P("sp", "tp"),
            P("sp", "tp"),
            P("tp", "sp"),
        ),
        out_specs=P(("grp", "sp", "tp"), None),
        check_vma=False,
    )
```

```python
import math

import jax
import jax.numpy as jnp
from jax import lax
from jax.experimental import pallas as pl
from jax.experimental.pallas import tpu as pltpu
from jax.sharding import PartitionSpec as P


HEAD_DIM = 64
LANES = 128


def gathered(resid_in, queries, keys, values, cum_gate, w_out, norm_gain, w_gate, w_up, w_down):
    tok_rows = queries.shape[0]
    local_heads = queries.shape[1] // HEAD_DIM
    scale = HEAD_DIM ** (-0.5)
    offset = lax.axis_index("sp") * tok_rows
    query_heads = queries.reshape(tok_rows, local_heads, HEAD_DIM)
    own_gate = lax.dynamic_slice_in_dim(cum_gate, offset, tok_rows, 0).T
    query_pos = offset + jnp.arange(tok_rows, dtype=jnp.int32)
    last_pos = offset + tok_rows - 1
    initial = (
        jnp.full((local_heads, tok_rows), -1e30, jnp.float32),
        jnp.zeros((local_heads, tok_rows), jnp.float32),
        jnp.zeros((tok_rows, local_heads, HEAD_DIM), jnp.float32),
    )
    key_piece = lax.all_gather(keys, "sp", axis=0, tiled=True)
    value_piece = lax.all_gather(values, "sp", axis=0, tiled=True)
    length = key_piece.shape[0]
    span = math.gcd(length, 512)

    def block(index, state):
        begin = index * span

        def work(inner):
            maxima, totals, summed = inner
            key_block = lax.dynamic_slice_in_dim(key_piece, index * span, span, 0).reshape(
                span, local_heads, HEAD_DIM
            )
            value_block_rows = lax.dynamic_slice_in_dim(value_piece, index * span, span, 0).reshape(
                span, local_heads, HEAD_DIM
            )
            key_gate = lax.dynamic_slice_in_dim(cum_gate, begin, span, 0).T
            scores = (
                jnp.einsum(
                    "qhd,khd->hqk", query_heads, key_block, preferred_element_type=jnp.float32
                )
                * scale
            )
            scores = scores + own_gate[:, :, None] - key_gate[:, None, :]
            key_pos = begin + jnp.arange(span, dtype=jnp.int32)
            mask = (key_pos[None, :] <= query_pos[:, None])[None]
            scores = jnp.where(mask, scores, -1e30)
            new_max = jnp.maximum(maxima, jnp.max(scores, axis=-1))
            weights = jnp.where(mask, jnp.exp(scores - new_max[:, :, None]), 0.0)
            rescale = jnp.exp(maxima - new_max)
            totals = totals * rescale + jnp.sum(weights, axis=-1)
            product = jnp.einsum(
                "hqk,khd->qhd",
                weights.astype(jnp.bfloat16),
                value_block_rows,
                preferred_element_type=jnp.float32,
            )
            summed = summed * rescale.T[:, :, None] + product
            return (new_max, totals, summed)

        return lax.cond(begin <= last_pos, work, lambda inner: inner, state)

    _, totals, summed = lax.fori_loop(0, length // span, block, initial)
    attended = (
        (summed / totals.T[:, :, None])
        .reshape(tok_rows, local_heads * HEAD_DIM)
        .astype(jnp.bfloat16)
    )
    head_rows = lax.all_to_all(attended, "tp", split_axis=0, concat_axis=1, tiled=True)
    mixed = jnp.dot(head_rows, w_out, preferred_element_type=jnp.float32)
    resid = resid_in.astype(jnp.float32) + mixed
    normed = resid * lax.rsqrt(jnp.mean(resid * resid, axis=-1, keepdims=True) + 1e-06)
    normed = (normed * norm_gain).astype(jnp.bfloat16)
    all_rows = lax.all_gather(normed, "tp", axis=0, tiled=True)
    full_gate, full_up, full_down = (
        lax.all_gather(w_gate, "sp", axis=0, tiled=True),
        lax.all_gather(w_up, "sp", axis=0, tiled=True),
        lax.all_gather(w_down, "sp", axis=1, tiled=True),
    )
    gate = jnp.dot(all_rows, full_gate, preferred_element_type=jnp.float32)
    up = jnp.dot(all_rows, full_up, preferred_element_type=jnp.float32)
    hidden = (jax.nn.silu(gate) * up).astype(jnp.bfloat16)
    terms = jnp.dot(hidden, full_down, preferred_element_type=jnp.float32)
    back = lax.psum_scatter(
        terms.astype(jnp.bfloat16), "tp", scatter_dimension=0, tiled=True
    ).astype(jnp.float32)
    return (resid + back).astype(jnp.bfloat16)


def splits(sizes, width, units, depth):
    if sizes["grp"] != 2 or sizes["tp"] != 4 or units % LANES:
        return False
    tiles = units // LANES
    per = -(-tiles // sizes["sp"])
    half = depth // 2
    span = per * LANES
    extra = span - half
    return (
        per * (sizes["sp"] - 1) < tiles
        and depth % (4 * LANES) == 0
        and extra > 0
        and half % extra == 0
        and width == depth * sizes["sp"]
    )


VMEM = pl.BlockSpec(memory_space=pltpu.VMEM)
SMEM = pl.BlockSpec(memory_space=pltpu.SMEM)
ANY = pl.BlockSpec(memory_space=pl.ANY)


def pack(place, keys, values, w_gate, w_up, w_down, sp, span):
    depth, units = w_gate.shape
    half = depth // 2
    tiles = units // LANES
    per = span // LANES
    extra = span - half
    rows, width = keys.shape

    def body(place_ref, key_ref, value_ref, gate_ref, up_ref, down_ref, *rest):
        outs, pair_ref, sem = rest[:sp], rest[sp], rest[sp + 1]
        s, g = place_ref[0], place_ref[1]
        copies = []

        def put(src, dst):
            copy = pltpu.make_async_copy(src, dst, sem)
            copy.start()
            copies.append(copy)

        def piece(out, dest, which):
            start = pl.multiple_of(jnp.minimum(per * dest, tiles - per) * LANES, LANES)
            row = pl.multiple_of(which * half, LANES)
            put(gate_ref.at[pl.ds(row, half), pl.ds(start, span)], out.at[pl.ds(0, half), :])
            put(up_ref.at[pl.ds(row, half), pl.ds(start, span)], out.at[pl.ds(half, half), :])
            put(
                down_ref.at[pl.ds(start, half), pl.ds(row, half)],
                out.at[pl.ds(2 * half, half), pl.ds(0, half)],
            )
            low = pl.multiple_of(start + half, LANES)
            for j in range(half // extra):
                col = pl.multiple_of(row + j * extra, LANES)
                put(
                    down_ref.at[pl.ds(low, extra), pl.ds(col, extra)],
                    out.at[pl.ds(2 * half + j * extra, extra), pl.ds(half, extra)],
                )

        put(key_ref, pair_ref.at[pl.ds(0, rows), :])
        put(value_ref, pair_ref.at[pl.ds(rows, rows), :])
        for k in range(1, sp):
            piece(outs[k], lax.rem(s + k, sp), g)
        for which in range(2):
            piece(outs[0].at[which], s, which)
        for copy in copies:
            copy.wait()

    shape = jax.ShapeDtypeStruct((3 * half, span), w_gate.dtype)
    return pl.pallas_call(
        body,
        in_specs=[SMEM] + [ANY] * 5,
        out_specs=[VMEM] * (sp + 1),
        out_shape=[jax.ShapeDtypeStruct((2, 3 * half, span), w_gate.dtype)]
        + [shape] * (sp - 1)
        + [jax.ShapeDtypeStruct((2 * rows, width), keys.dtype)],
        scratch_shapes=[pltpu.SemaphoreType.DMA],
        name="pack",
    )(place, keys, values, w_gate, w_up, w_down)


def attend(place, queries, pairs, cum_gate, gate_rows):
    rows, width = queries.shape
    heads = width // HEAD_DIM
    blocks = len(pairs)
    scale = HEAD_DIM ** (-0.5)

    def body(place_ref, q_ref, *rest):
        pair_refs, cum_ref, gate_ref, out_ref = rest[:blocks], *rest[blocks:]
        s = place_ref[0]
        query = q_ref[...] * jnp.asarray(scale, q_ref.dtype)
        lane = lax.broadcasted_iota(jnp.int32, (rows, width), 1) // HEAD_DIM
        row_id = lax.broadcasted_iota(jnp.int32, (rows, rows), 0)
        col_id = lax.broadcasted_iota(jnp.int32, (rows, rows), 1)
        own = cum_ref[pl.ds(pl.multiple_of(s * rows, LANES), rows), :]
        result = jnp.zeros((rows, width), jnp.float32)
        for h in range(heads):
            one = jnp.where(lane == h, query, jnp.zeros_like(query))
            scores = []
            for k in range(blocks):
                keys = pair_refs[k][0:rows, :]
                score = lax.dot_general(
                    one, keys, (((1,), (1,)), ((), ())), preferred_element_type=jnp.float32
                )
                at = pl.multiple_of(lax.rem(s - k + blocks, blocks) * rows, LANES)
                score = score + own[:, h : h + 1] - gate_ref[h : h + 1, pl.ds(at, rows)]
                keep = (col_id <= row_id) if k == 0 else (jnp.full((1, 1), s - k, jnp.int32) >= 0)
                scores.append(jnp.where(keep, score, -1e30))
            top = scores[0].max(axis=-1, keepdims=True)
            for k in range(1, blocks):
                top = jnp.maximum(top, scores[k].max(axis=-1, keepdims=True))
            total = jnp.zeros((rows, 1), jnp.float32)
            summed = jnp.zeros((rows, width), jnp.float32)
            for k in range(blocks):
                weight = jnp.exp(scores[k] - top)
                total = total + weight.sum(axis=-1, keepdims=True)
                summed = summed + jnp.dot(
                    weight.astype(jnp.bfloat16),
                    pair_refs[k][rows : 2 * rows, :],
                    preferred_element_type=jnp.float32,
                )
            result = jnp.where(lane == h, summed / total, result)
        out_ref[...] = result.astype(out_ref.dtype)

    return pl.pallas_call(
        body,
        in_specs=[SMEM] + [VMEM] * (blocks + 3),
        out_specs=VMEM,
        out_shape=jax.ShapeDtypeStruct((rows, width), jnp.bfloat16),
        name="attend",
    )(place, queries, *pairs, cum_gate, gate_rows)


def feed(place, mine, other, pieces, tiles, span):
    sp = len(mine)
    block, width = mine[0].shape
    depth = width // sp
    half = depth // 2
    extra = span - half
    rows = 2 * sp * block
    cols = 2 * span
    per = span // LANES
    arrays = [p[4] for p in pieces]

    def body(place_ref, *rest):
        row_refs = rest[: 2 * sp]
        piece_refs = rest[2 * sp : 2 * sp + len(arrays)]
        own_ref, other_ref, x_ref, gate_ref, up_ref, down_ref, sems = rest[2 * sp + len(arrays) :]
        s, g = place_ref[0], place_ref[1]
        copies = [[], [], [], []]

        def put(src, dst, n):
            copy = pltpu.make_async_copy(src, dst, sems.at[n])
            copy.start()
            copies[n].append(copy)

        for j, ref in enumerate(row_refs):
            put(ref, x_ref.at[pl.ds(j * block, block), :], 0)

        def spread(stage):
            for (k, which, column, first, _), ref in zip(pieces, piece_refs, strict=True):
                for n in range(2) if which is None else (which,):
                    src = ref.at[n] if which is None else ref
                    part = n if which is None else (g if n == 0 else 1 - g)
                    at = pl.multiple_of(lax.rem(s - k + sp, sp) * depth + part * half, LANES)
                    col = column * span
                    low = max(first, (stage - 1) * half)
                    high = min(first + src.shape[0], stage * half)
                    if low >= high:
                        continue
                    skip, count = low - (stage - 1) * half, high - low
                    if stage < 3:
                        full = gate_ref if stage == 1 else up_ref
                        put(
                            src.at[pl.ds(low - first, count), :],
                            full.at[pl.ds(at + skip, count), pl.ds(col, span)],
                            stage,
                        )
                        continue
                    put(
                        src.at[pl.ds(low - first, half), pl.ds(0, half)],
                        down_ref.at[pl.ds(col, half), pl.ds(at, half)],
                        3,
                    )
                    for j in range(half // extra):
                        put(
                            src.at[pl.ds(low - first + j * extra, extra), pl.ds(half, extra)],
                            down_ref.at[
                                pl.ds(col + half, extra),
                                pl.ds(pl.multiple_of(at + j * extra, LANES), extra),
                            ],
                            3,
                        )

        for stage in (1, 2, 3):
            spread(stage)
        for n in (0, 1):
            for copy in copies[n]:
                copy.wait()
        gate = jnp.dot(x_ref[...], gate_ref[...], preferred_element_type=jnp.float32)
        for copy in copies[2]:
            copy.wait()
        up = jnp.dot(x_ref[...], up_ref[...], preferred_element_type=jnp.float32)
        hidden = gate / (1.0 + jnp.exp(-gate)) * up
        again = per * s - jnp.minimum(per * s, tiles - per)
        unit = lax.broadcasted_iota(jnp.int32, (rows, cols), 1)
        unit = jnp.where(unit >= span, unit - span, unit)
        hidden = jnp.where(unit >= again * LANES, hidden, 0.0).astype(jnp.bfloat16)
        for copy in copies[3]:
            copy.wait()
        product = jnp.dot(hidden, down_ref[...], preferred_element_type=jnp.float32)
        own_ref[...] = product[: rows // 2]
        other_ref[...] = product[rows // 2 :].astype(other_ref.dtype)

    return pl.pallas_call(
        body,
        in_specs=[SMEM] + [ANY] * (2 * sp + len(arrays)),
        out_specs=[VMEM, VMEM],
        out_shape=[
            jax.ShapeDtypeStruct((rows // 2, width), jnp.float32),
            jax.ShapeDtypeStruct((rows // 2, width), jnp.bfloat16),
        ],
        scratch_shapes=[
            pltpu.VMEM((rows, width), jnp.bfloat16),
            pltpu.VMEM((width, cols), jnp.bfloat16),
            pltpu.VMEM((width, cols), jnp.bfloat16),
            pltpu.VMEM((cols, width), jnp.bfloat16),
            pltpu.SemaphoreType.DMA((4,)),
        ],
        name="feed",
    )(place, *mine, *other, *arrays)


def unit_slices(resid_in, queries, keys, values, cum_gate, w_out, norm_gain, w_gate, w_up, w_down):
    sp, tp = lax.axis_size("sp"), lax.axis_size("tp")
    tiles = w_gate.shape[1] // LANES
    span = -(-tiles // sp) * LANES
    place = jnp.stack([lax.axis_index("sp"), lax.axis_index("grp")]).astype(jnp.int32)

    def turn(a, k):
        return lax.ppermute(a, "sp", [(i, (i + k) % sp) for i in range(sp)])

    def later(a, k):
        return lax.ppermute(a, "sp", [(i, i + k) for i in range(sp - k)])

    def flip(a, m):
        return lax.ppermute(a, "tp", [(i, i ^ m) for i in range(tp)])

    def swap(a):
        return lax.ppermute(a, "grp", [(0, 1), (1, 0)])

    across, core = tp // 2, 1
    *packed, pair = pack(place, keys, values, w_gate, w_up, w_down, sp, span)
    pieces = [(0, None, 0, 0, packed[0]), (0, None, 1, 0, flip(packed[0], across))]
    pairs = [pair] + [later(pair, k) for k in range(1, sp)]
    mid = packed[1].shape[0] // 2
    for k in range(1, sp):
        here = turn(packed[k], k)
        there = flip(here, across)
        twin = swap(here)
        pieces += [
            (k, 0, 0, 0, here),
            (k, 1, 0, 0, twin),
            (k, 0, 1, 0, there),
            (k, 1, 1, 0, flip(twin[:mid], across)),
            (k, 1, 1, mid, swap(there[mid:])),
        ]

    attended = attend(place, queries, pairs, cum_gate, cum_gate.T)
    head_rows = lax.all_to_all(attended, "tp", split_axis=0, concat_axis=1, tiled=True)
    mixed = jnp.dot(head_rows, w_out, preferred_element_type=jnp.float32)
    resid = resid_in.astype(jnp.float32) + mixed
    normed = resid * lax.rsqrt(jnp.mean(resid * resid, axis=-1, keepdims=True) + 1e-06)
    normed = (normed * norm_gain).astype(jnp.bfloat16)

    mine = [normed] + [turn(normed, k) for k in range(1, sp)]
    other = [flip(a, core) for a in mine]
    own, away = feed(place, mine, other, pieces, tiles, span)
    total = own + flip(away, core).astype(jnp.float32)
    total = total.reshape(sp, -1, total.shape[1])
    result = resid + total[0]
    for k in range(1, sp):
        piece = turn(total[k].astype(jnp.bfloat16), sp - k)
        result = result + piece.astype(jnp.float32)
    return result.astype(jnp.bfloat16)


def on_device(*arrays):
    sizes = {name: lax.axis_size(name) for name in ("grp", "sp", "tp")}
    w_out, w_gate = arrays[5], arrays[7]
    if splits(sizes, w_out.shape[1], w_gate.shape[1], w_gate.shape[0]):
        return unit_slices(*arrays)
    return gathered(*arrays)


def solution(mesh):
    return jax.shard_map(
        on_device,
        mesh=mesh,
        in_specs=(
            P(("grp", "sp", "tp"), None),
            P(("grp", "sp"), "tp"),
            P(("grp", "sp"), "tp"),
            P(("grp", "sp"), "tp"),
            P("grp", "tp"),
            P(),
            P(),
            P("sp", "tp"),
            P("sp", "tp"),
            P("tp", "sp"),
        ),
        out_specs=P(("grp", "sp", "tp"), None),
        check_vma=False,
    )
```
